32 devices in a mesh: sp: 16 (over z, y, x), dp: 2 (over core).
Axes of the slice: x: 2, y: 2, z: 4, core: 2. Of those that a mesh axis runs over, the one named last changes fastest.
Arguments:
- gate_input: bfloat16 [2, 3072, 1024], P('dp', 'sp'), may hold values from -6 to 6
- value_input: bfloat16 [2, 3072, 1024], P('dp', 'sp'), may hold values from -6 to 6
- norm_gain: float32 [1024], replicated, may hold values from 0.1 to 1.9
- norm_bias: float32 [1024], replicated, may hold values from -3 to 3
- mix_weight: bfloat16 [16, 1024, 1024], P('sp', 'dp'), may hold values from -0.1875 to 0.1875
- mix_bias: float32 [16, 1024], P('sp'), may hold values from 0.1 to 1.9
Outputs:
- gated: bfloat16 [2, 3072, 1024], P('dp', 'sp')
The draws below stay inside these ranges and needn't reach their ends.
All inputs are finite; a program needn't handle non-finite values.
Results may differ from the reference program's by a relative error of at most 0.0053.
Values may be sent and summed in bfloat16 or wider, within the bound.
A program may use at most 64 MiB of HBM per device.

```python
import jax
import jax.numpy as jnp
from jax import lax

GROUP_DIM = 64
SPAN = 1024
GROUPS = 16
WIDTH = 1024
SEQ = 3072
BATCH = 2


def shard_levels(own_key, dims, shards, least, largest):
    def one(position, blocks):
        steps = jax.random.uniform(jax.random.fold_in(jax.random.fold_in(own_key, 6), position), (blocks,), jnp.float32, least / len(shards), largest / len(shards))
        return jnp.repeat(jnp.exp(steps), dims[position] // blocks).reshape((-1,) + (1,) * (len(dims) - position - 1))

    loudness = one(*shards[0])
    for cut in shards[1:]:
        loudness = loudness * one(*cut)
    return loudness


def gaussian(own_key, shape, width, limit, cuts=(), dtype=jnp.bfloat16):
    drawn = jax.random.normal(own_key, shape, jnp.float32) * width
    if len(cuts) > 0:
        drawn = shard_levels(own_key, shape, cuts, -0.22, 0.18) * drawn
    return jnp.clip(drawn, min=-limit, max=limit).astype(dtype)


def setup_inputs(seed: int = 0) -> dict:
    key_list = jax.random.split(jax.random.key(seed), 7)
    gate_input = gaussian(key_list[0], (BATCH, SEQ, WIDTH), 1.0, 6.0, ((0, 2), (1, 16)))
    value_input = gaussian(key_list[1], (BATCH, SEQ, WIDTH), 1.0, 6.0, ((0, 2), (1, 16)))
    norm_gain = jnp.clip(1.0 + 0.18 * jax.random.normal(key_list[2], (WIDTH,), jnp.float32), 0.1, 1.9)
    norm_bias = gaussian(key_list[3], (WIDTH,), 0.5, 3.0, (), jnp.float32)
    mix_weight = gaussian(key_list[4], (GROUPS, SPAN, SPAN), SPAN ** -0.5, 0.1875, ((0, 16), (1, 2)))
    mix_bias = jnp.clip(1.0 + 0.18 * jax.random.normal(key_list[5], (GROUPS, SPAN), jnp.float32), 0.1, 1.9)
    return dict(gate_input=gate_input, value_input=value_input, norm_gain=norm_gain, norm_bias=norm_bias, mix_weight=mix_weight, mix_bias=mix_bias)


epsilon = 1e-05

def reference(gate_input, value_input, norm_gain, norm_bias, mix_weight, mix_bias):
    causal = jnp.tril(jnp.ones((SPAN, SPAN), jnp.float32))
    weight = mix_weight.astype(jnp.float32) * causal[None]

    def per_sequence(inputs):
        gate_rows, value_rows = inputs
        act_value = jax.nn.gelu(value_rows.astype(jnp.float32))
        centre = lax.optimization_barrier(jnp.mean(act_value, axis=-1, keepdims=True))
        shifted = act_value - centre
        variance = lax.optimization_barrier(jnp.mean(shifted * shifted, axis=-1, keepdims=True))
        normed = (shifted * lax.rsqrt(variance + epsilon) * norm_gain + norm_bias).astype(jnp.bfloat16)
        blocks = normed.astype(jnp.float32).reshape(SEQ // SPAN, SPAN, GROUPS, GROUP_DIM)
        summed = jnp.einsum('gqp,npgc->nqgc', weight, blocks, precision=lax.Precision.HIGHEST)
        mixed_rows = (summed + mix_bias.T[None, :, :, None]).reshape(SEQ, WIDTH).astype(jnp.bfloat16)
        mixed_rows = lax.optimization_barrier(mixed_rows)
        act_gate = jax.nn.gelu(gate_rows.astype(jnp.float32))
        return (act_gate * mixed_rows.astype(jnp.float32)).astype(jnp.bfloat16)
    return lax.map(per_sequence, (gate_input, value_input))
```

```python
import functools
import math

import jax
import jax.numpy as jnp
from jax import lax
from jax.experimental import pallas as pl
from jax.experimental.pallas import tpu as pltpu
from jax.sharding import PartitionSpec as P

GROUP_DIM = 64
SPAN = 1024
LANES = 128
ROWS = 16

epsilon = 1e-05


def partner(me, k, n):
    if n & (n - 1):
        return lax.rem(me + k, n)
    out = 0
    bit = 1
    while bit < n:
        flip = 1 if k & bit else 0
        out = out + ((me // bit + flip) % 2) * bit
        bit *= 2
    return out


def segments(source, rows):
    half = rows // 2
    runs = []
    for a in range(2):
        r = 0
        while r < half:
            position = source * rows + a * half + r
            block, p = divmod(position, SPAN)
            length = min(half - r, SPAN - p)
            runs.append((a, r, length, block, p))
            r += length
    return runs


def kernel(
    n, dp, tile, value, gate, gain, nbias, weight, mbias, out,
    vbuf, gbuf, gainbuf, nbiasbuf, mbiasbuf, act, full, bcol, s1, r1, xbuf, ybuf, s2, r2, obuf,
    load_sem, wsend, wrecv, send1, recv1, send2, recv2, out_sem,
):
    me = lax.axis_index("sp")
    row = lax.axis_index("dp")
    tokens, channels = vbuf.shape
    half = tokens // 2
    wrows = weight.shape[0]
    pairs = channels // LANES

    load_value = pltpu.make_async_copy(value, vbuf, load_sem.at[0])
    load_gain = pltpu.make_async_copy(gain, gainbuf, load_sem.at[1])
    load_nbias = pltpu.make_async_copy(nbias, nbiasbuf, load_sem.at[2])
    load_gate = pltpu.make_async_copy(gate, gbuf, load_sem.at[3])
    load_mbias = pltpu.make_async_copy(mbias, mbiasbuf, load_sem.at[4])
    own_rows = full.at[pl.ds(pl.multiple_of(row * wrows, wrows), wrows), :]
    load_weight = pltpu.make_async_copy(weight, own_rows, load_sem.at[5])
    load_value.start()
    load_gain.start()
    load_nbias.start()
    load_weight.start()
    load_mbias.start()
    load_gate.start()

    barrier = pltpu.get_barrier_semaphore()
    order = list(range(n - 1, 0, -1))
    peers = {k: partner(me, k, n) for k in order}
    for k in order:
        pl.semaphore_signal(barrier, inc=1, device_id={"sp": peers[k]})
    for j in range(1, dp):
        pl.semaphore_signal(barrier, inc=1, device_id={"dp": lax.rem(row + j, dp)})

    load_value.wait()
    load_gain.wait()
    load_nbias.wait()
    lower = lax.broadcasted_iota(jnp.int32, (ROWS, LANES), 1) < GROUP_DIM

    def normed_rows(start):
        x = jax.nn.gelu(vbuf[pl.ds(start, ROWS), :].astype(jnp.float32))
        shifted = x - jnp.mean(x, axis=-1, keepdims=True)
        variance = jnp.mean(shifted * shifted, axis=-1, keepdims=True)
        return shifted * lax.rsqrt(variance + epsilon) * gainbuf[...] + nbiasbuf[...]

    for r in range(0, half, ROWS):
        top = normed_rows(r)
        bottom = normed_rows(half + r)
        for j in range(pairs):
            t = top[:, j * LANES:(j + 1) * LANES]
            b = bottom[:, j * LANES:(j + 1) * LANES]
            s1[2 * j, pl.ds(r, ROWS), :] = jnp.where(lower, t, pltpu.roll(b, GROUP_DIM, 1)).astype(jnp.bfloat16)
            s1[2 * j + 1, pl.ds(r, ROWS), :] = jnp.where(lower, pltpu.roll(t, GROUP_DIM, 1), b).astype(jnp.bfloat16)

    pl.semaphore_wait(barrier, n - 1 + dp - 1)

    def exchange(src, dst, send_sem, recv_sem):
        copies = []
        for k in order:
            copy = pltpu.make_async_remote_copy(
                src_ref=src.at[peers[k]], dst_ref=dst.at[me], send_sem=send_sem.at[k],
                recv_sem=recv_sem.at[me], device_id={"sp": peers[k]},
            )
            copy.start()
            copies.append(copy)
        pltpu.make_async_copy(src.at[me], dst.at[me], recv_sem.at[me]).start()
        return copies

    sends = exchange(s1, r1, send1, recv1)
    wcopies = []
    for j in range(1, dp):
        copy = pltpu.make_async_remote_copy(
            src_ref=weight, dst_ref=own_rows, send_sem=wsend.at[j], recv_sem=wrecv.at[row],
            device_id={"dp": lax.rem(row + j, dp)},
        )
        copy.start()
        wcopies.append(copy)

    load_gate.wait()
    for r in range(0, tokens, ROWS):
        act[pl.ds(r, ROWS), :] = jax.nn.gelu(gbuf[pl.ds(r, ROWS), :].astype(jnp.float32))
    load_mbias.wait()
    for q in range(0, SPAN, LANES):
        bcol[pl.ds(q, LANES), :] = jnp.transpose(jnp.broadcast_to(mbiasbuf[:, q:q + LANES], (LANES, LANES)))
    xbuf[:, xbuf.shape[1] - LANES:] = jnp.zeros((SPAN, LANES), jnp.bfloat16)

    load_weight.wait()
    for j in range(1, dp):
        other = lax.rem(row + j, dp)
        rows_of = full.at[pl.ds(pl.multiple_of(other * wrows, wrows), wrows), :]
        pltpu.make_async_copy(weight, rows_of, wrecv.at[other]).wait()
    for q in range(0, SPAN, tile):
        block = full[pl.ds(q, tile), pl.ds(q, tile)].astype(jnp.float32)
        keep = lax.broadcasted_iota(jnp.int32, (tile, tile), 1) <= lax.broadcasted_iota(jnp.int32, (tile, tile), 0)
        full[pl.ds(q, tile), pl.ds(q, tile)] = jnp.where(keep, block, 0.0).astype(jnp.bfloat16)

    for s in range(n):
        pltpu.make_async_copy(s1.at[s], r1.at[s], recv1.at[s]).wait()
        for a, r, length, block, p in segments(s, tokens):
            xbuf[p:p + length, block * GROUP_DIM:(block + 1) * GROUP_DIM] = (
                r1[s, r:r + length, a * GROUP_DIM:(a + 1) * GROUP_DIM]
            )

    for q in range(0, SPAN, tile):
        summed = jnp.dot(full[q:q + tile, :q + tile], xbuf[:q + tile, :], preferred_element_type=jnp.float32)
        column = bcol[q:q + tile, :]
        for j in range(0, xbuf.shape[1], LANES):
            ybuf[q:q + tile, j:j + LANES] = (summed[:, j:j + LANES] + column).astype(jnp.bfloat16)

    for s in range(n):
        for a, r, length, block, p in segments(s, tokens):
            s2[s, r:r + length, a * GROUP_DIM:(a + 1) * GROUP_DIM] = (
                ybuf[p:p + length, block * GROUP_DIM:(block + 1) * GROUP_DIM]
            )
    returns = exchange(s2, r2, send2, recv2)

    stores = []
    for j in range(pairs):
        for s in (2 * j, 2 * j + 1):
            pltpu.make_async_copy(s2.at[s], r2.at[s], recv2.at[s]).wait()
        cols = slice(j * LANES, (j + 1) * LANES)
        for r in range(0, half, ROWS):
            e = r2[2 * j, r:r + ROWS, :].astype(jnp.float32)
            o = r2[2 * j + 1, r:r + ROWS, :].astype(jnp.float32)
            top = jnp.where(lower, e, pltpu.roll(o, GROUP_DIM, 1))
            bottom = jnp.where(lower, pltpu.roll(e, GROUP_DIM, 1), o)
            obuf[r:r + ROWS, cols] = (act[r:r + ROWS, cols] * top).astype(jnp.bfloat16)
            obuf[half + r:half + r + ROWS, cols] = (act[half + r:half + r + ROWS, cols] * bottom).astype(jnp.bfloat16)
    store = pltpu.make_async_copy(obuf, out, out_sem.at[0])
    store.start()
    for copy in sends + wcopies + returns:
        copy.wait_send()
    store.wait()


def solution(mesh):
    n, dp = mesh.shape["sp"], mesh.shape["dp"]

    def local(gate_input, value_input, norm_gain, norm_bias, mix_weight, mix_bias):
        _, tokens, channels = value_input.shape
        groups, wrows, span = mix_weight.shape
        assert groups == 1 and span == SPAN and channels == n * GROUP_DIM and tokens % (2 * ROWS) == 0
        half = tokens // 2
        blocks = n * tokens // SPAN
        width = -(-blocks * GROUP_DIM // LANES) * LANES
        packed = (n, half, 2 * GROUP_DIM)
        anywhere = pl.BlockSpec(memory_space=pl.ANY)
        bf16, f32 = jnp.bfloat16, jnp.float32
        dma = pltpu.SemaphoreType.DMA
        result = pl.pallas_call(
            functools.partial(kernel, n, dp, 256),
            out_shape=jax.ShapeDtypeStruct((tokens, channels), bf16),
            in_specs=[anywhere] * 6,
            out_specs=anywhere,
            scratch_shapes=[
                pltpu.VMEM((tokens, channels), bf16),
                pltpu.VMEM((tokens, channels), bf16),
                pltpu.VMEM((1, channels), f32),
                pltpu.VMEM((1, channels), f32),
                pltpu.VMEM((1, SPAN), f32),
                pltpu.VMEM((tokens, channels), f32),
                pltpu.VMEM((SPAN, SPAN), bf16),
                pltpu.VMEM((SPAN, LANES), f32),
                pltpu.VMEM(packed, bf16),
                pltpu.VMEM(packed, bf16),
                pltpu.VMEM((SPAN, width), bf16),
                pltpu.VMEM((SPAN, width), bf16),
                pltpu.VMEM(packed, bf16),
                pltpu.VMEM(packed, bf16),
                pltpu.VMEM((tokens, channels), bf16),
                dma((6,)),
                dma((dp,)),
                dma((dp,)),
                dma((n,)),
                dma((n,)),
                dma((n,)),
                dma((n,)),
                dma((1,)),
            ],
            compiler_params=pltpu.CompilerParams(collective_id=0, has_side_effects=True),
        )(
            value_input[0], gate_input[0], norm_gain.reshape(1, channels), norm_bias.reshape(1, channels),
            mix_weight[0], mix_bias,
        )
        return result.reshape(1, tokens, channels)

    in_specs = (
        P("dp", "sp", None),
        P("dp", "sp", None),
        P(),
        P(),
        P("sp", "dp", None),
        P("sp", None),
    )
    return jax.shard_map(local, mesh=mesh, in_specs=in_specs, out_specs=P("dp", "sp", None), check_vma=False)
```

```python
import functools
import math

import jax
import jax.numpy as jnp
from jax import lax
from jax.experimental import pallas as pl
from jax.experimental.pallas import tpu as pltpu
from jax.sharding import PartitionSpec as P

GROUP_DIM = 64
SPAN = 1024
LANES = 128
ROWS = 16

epsilon = 1e-05


def partner(me, k, n):
    if n & (n - 1):
        return lax.rem(me + k, n)
    out = 0
    bit = 1
    while bit < n:
        flip = 1 if k & bit else 0
        out = out + ((me // bit + flip) % 2) * bit
        bit *= 2
    return out


def segments(source, rows):
    half = rows // 2
    runs = []
    for a in range(2):
        r = 0
        while r < half:
            position = source * rows + a * half + r
            block, p = divmod(position, SPAN)
            length = min(half - r, SPAN - p)
            runs.append((a, r, length, block, p))
            r += length
    return runs


def kernel(
    n, dp, tile, value, gate, gain, nbias, weight, mbias, out,
    vbuf, gbuf, gainbuf, nbiasbuf, mbiasbuf, act, full, bcol, s1, r1, xbuf, ybuf, s2, r2,
    load_sem, wsend, wrecv, send1, recv1, send2, recv2,
):
    me = lax.axis_index("sp")
    row = lax.axis_index("dp")
    tokens, channels = vbuf.shape
    half = tokens // 2
    wrows = weight.shape[0]
    pairs = channels // LANES

    load_value = pltpu.make_async_copy(value, vbuf, load_sem.at[0])
    load_gain = pltpu.make_async_copy(gain, gainbuf, load_sem.at[1])
    load_nbias = pltpu.make_async_copy(nbias, nbiasbuf, load_sem.at[2])
    load_gate = pltpu.make_async_copy(gate, gbuf, load_sem.at[3])
    load_mbias = pltpu.make_async_copy(mbias, mbiasbuf, load_sem.at[4])
    own_rows = full.at[pl.ds(pl.multiple_of(row * wrows, wrows), wrows), :]
    load_weight = pltpu.make_async_copy(weight, own_rows, load_sem.at[5])
    load_value.start()
    load_gain.start()
    load_nbias.start()
    load_weight.start()
    load_mbias.start()
    load_gate.start()

    barrier = pltpu.get_barrier_semaphore()
    order = list(range(n - 1, 0, -1))
    peers = {k: partner(me, k, n) for k in order}
    for k in order:
        pl.semaphore_signal(barrier, inc=1, device_id={"sp": peers[k]})
    for j in range(1, dp):
        pl.semaphore_signal(barrier, inc=1, device_id={"dp": lax.rem(row + j, dp)})

    load_value.wait()
    load_gain.wait()
    load_nbias.wait()
    lower = lax.broadcasted_iota(jnp.int32, (ROWS, LANES), 1) < GROUP_DIM

    def normed_rows(start):
        x = jax.nn.gelu(vbuf[pl.ds(start, ROWS), :].astype(jnp.float32))
        shifted = x - jnp.mean(x, axis=-1, keepdims=True)
        variance = jnp.mean(shifted * shifted, axis=-1, keepdims=True)
        return shifted * lax.rsqrt(variance + epsilon) * gainbuf[...] + nbiasbuf[...]

    for r in range(0, half, ROWS):
        top = normed_rows(r)
        bottom = normed_rows(half + r)
        for j in range(pairs):
            t = top[:, j * LANES:(j + 1) * LANES]
            b = bottom[:, j * LANES:(j + 1) * LANES]
            s1[2 * j, pl.ds(r, ROWS), :] = jnp.where(lower, t, pltpu.roll(b, GROUP_DIM, 1)).astype(jnp.bfloat16)
            s1[2 * j + 1, pl.ds(r, ROWS), :] = jnp.where(lower, pltpu.roll(t, GROUP_DIM, 1), b).astype(jnp.bfloat16)

    pl.semaphore_wait(barrier, n - 1 + dp - 1)

    def exchange(src, dst, send_sem, recv_sem):
        copies = []
        for k in order:
            copy = pltpu.make_async_remote_copy(
                src_ref=src.at[peers[k]], dst_ref=dst.at[me], send_sem=send_sem.at[k],
                recv_sem=recv_sem.at[me], device_id={"sp": peers[k]},
            )
            copy.start()
            copies.append(copy)
        pltpu.make_async_copy(src.at[me], dst.at[me], recv_sem.at[me]).start()
        return copies

    sends = exchange(s1, r1, send1, recv1)
    wcopies = []
    for j in range(1, dp):
        copy = pltpu.make_async_remote_copy(
            src_ref=weight, dst_ref=own_rows, send_sem=wsend.at[j], recv_sem=wrecv.at[row],
            device_id={"dp": lax.rem(row + j, dp)},
        )
        copy.start()
        wcopies.append(copy)

    load_gate.wait()
    for r in range(0, tokens, ROWS):
        act[pl.ds(r, ROWS), :] = jax.nn.gelu(gbuf[pl.ds(r, ROWS), :].astype(jnp.float32))
    load_mbias.wait()
    for q in range(0, SPAN, LANES):
        bcol[pl.ds(q, LANES), :] = jnp.transpose(jnp.broadcast_to(mbiasbuf[:, q:q + LANES], (LANES, LANES)))
    xbuf[:, xbuf.shape[1] - LANES:] = jnp.zeros((SPAN, LANES), jnp.bfloat16)

    load_weight.wait()
    for j in range(1, dp):
        other = lax.rem(row + j, dp)
        rows_of = full.at[pl.ds(pl.multiple_of(other * wrows, wrows), wrows), :]
        pltpu.make_async_copy(weight, rows_of, wrecv.at[other]).wait()
    for q in range(0, SPAN, tile):
        block = full[pl.ds(q, tile), pl.ds(q, tile)].astype(jnp.float32)
        keep = lax.broadcasted_iota(jnp.int32, (tile, tile), 1) <= lax.broadcasted_iota(jnp.int32, (tile, tile), 0)
        full[pl.ds(q, tile), pl.ds(q, tile)] = jnp.where(keep, block, 0.0).astype(jnp.bfloat16)

    for s in range(n):
        pltpu.make_async_copy(s1.at[s], r1.at[s], recv1.at[s]).wait()
        for a, r, length, block, p in segments(s, tokens):
            xbuf[p:p + length, block * GROUP_DIM:(block + 1) * GROUP_DIM] = (
                r1[s, r:r + length, a * GROUP_DIM:(a + 1) * GROUP_DIM]
            )

    for q in range(0, SPAN, tile):
        summed = jnp.dot(full[q:q + tile, :q + tile], xbuf[:q + tile, :], preferred_element_type=jnp.float32)
        column = bcol[q:q + tile, :]
        for j in range(0, xbuf.shape[1], LANES):
            ybuf[q:q + tile, j:j + LANES] = (summed[:, j:j + LANES] + column).astype(jnp.bfloat16)

    for s in range(n):
        for a, r, length, block, p in segments(s, tokens):
            s2[s, r:r + length, a * GROUP_DIM:(a + 1) * GROUP_DIM] = (
                ybuf[p:p + length, block * GROUP_DIM:(block + 1) * GROUP_DIM]
            )
    returns = exchange(s2, r2, send2, recv2)

    for j in range(pairs):
        for s in (2 * j, 2 * j + 1):
            pltpu.make_async_copy(s2.at[s], r2.at[s], recv2.at[s]).wait()
        cols = slice(j * LANES, (j + 1) * LANES)
        for r in range(0, half, ROWS):
            e = r2[2 * j, r:r + ROWS, :].astype(jnp.float32)
            o = r2[2 * j + 1, r:r + ROWS, :].astype(jnp.float32)
            top = jnp.where(lower, e, pltpu.roll(o, GROUP_DIM, 1))
            bottom = jnp.where(lower, pltpu.roll(e, GROUP_DIM, 1), o)
            out[r:r + ROWS, cols] = (act[r:r + ROWS, cols] * top).astype(jnp.bfloat16)
            out[half + r:half + r + ROWS, cols] = (act[half + r:half + r + ROWS, cols] * bottom).astype(jnp.bfloat16)
    for copy in sends + wcopies + returns:
        copy.wait_send()


def solution(mesh):
    n, dp = mesh.shape["sp"], mesh.shape["dp"]

    def local(gate_input, value_input, norm_gain, norm_bias, mix_weight, mix_bias):
        _, tokens, channels = value_input.shape
        groups, wrows, span = mix_weight.shape
        assert groups == 1 and span == SPAN and channels == n * GROUP_DIM and tokens % (2 * ROWS) == 0
        half = tokens // 2
        blocks = n * tokens // SPAN
        width = -(-blocks * GROUP_DIM // LANES) * LANES
        packed = (n, half, 2 * GROUP_DIM)
        anywhere = pl.BlockSpec(memory_space=pl.ANY)
        bf16, f32 = jnp.bfloat16, jnp.float32
        dma = pltpu.SemaphoreType.DMA
        result = pl.pallas_call(
            functools.partial(kernel, n, dp, 256),
            out_shape=pltpu.VMEM((tokens, channels), bf16),
            in_specs=[anywhere] * 6,
            out_specs=pl.BlockSpec(memory_space=pltpu.VMEM),
            scratch_shapes=[
                pltpu.VMEM((tokens, channels), bf16),
                pltpu.VMEM((tokens, channels), bf16),
                pltpu.VMEM((1, channels), f32),
                pltpu.VMEM((1, channels), f32),
                pltpu.VMEM((1, SPAN), f32),
                pltpu.VMEM((tokens, channels), f32),
                pltpu.VMEM((SPAN, SPAN), bf16),
                pltpu.VMEM((SPAN, LANES), f32),
                pltpu.VMEM(packed, bf16),
                pltpu.VMEM(packed, bf16),
                pltpu.VMEM((SPAN, width), bf16),
                pltpu.VMEM((SPAN, width), bf16),
                pltpu.VMEM(packed, bf16),
                pltpu.VMEM(packed, bf16),
                dma((6,)),
                dma((dp,)),
                dma((dp,)),
                dma((n,)),
                dma((n,)),
                dma((n,)),
                dma((n,)),
            ],
            compiler_params=pltpu.CompilerParams(collective_id=0, has_side_effects=True),
        )(
            value_input[0], gate_input[0], norm_gain.reshape(1, channels), norm_bias.reshape(1, channels),
            mix_weight[0], mix_bias,
        )
        return result.reshape(1, tokens, channels)

    in_specs = (
        P("dp", "sp", None),
        P("dp", "sp", None),
        P(),
        P(),
        P("sp", "dp", None),
        P("sp", None),
    )
    return jax.shard_map(local, mesh=mesh, in_specs=in_specs, out_specs=P("dp", "sp", None), check_vma=False)
```

```python
import functools
import math

import jax
import jax.numpy as jnp
from jax import lax
from jax.experimental import pallas as pl
from jax.experimental.pallas import tpu as pltpu
from jax.sharding import PartitionSpec as P

GROUP_DIM = 64
SPAN = 1024
LANES = 128
ROWS = 16

epsilon = 1e-05


def partner(me, k, n):
    if n & (n - 1):
        return lax.rem(me + k, n)
    out = 0
    bit = 1
    while bit < n:
        out = out + ((me // bit + k // bit) % 2) * bit
        bit *= 2
    return out


def segments(source, rows):
    half = rows // 2
    runs = []
    for a in range(2):
        r = 0
        while r < half:
            position = source * rows + a * half + r
            block, p = divmod(position, SPAN)
            length = min(half - r, SPAN - p)
            runs.append((a, r, length, block, p))
            r += length
    return runs


def kernel(
    n, dp, tile, value, gate, gain, nbias, weight, mbias, out,
    vbuf, gbuf, gainbuf, nbiasbuf, mbiasbuf, act, full, bcol, s1, r1, xbuf, ybuf, s2, r2,
    load_sem, wsend, wrecv, send1, recv1, send2, recv2,
):
    me = lax.axis_index("sp")
    row = lax.axis_index("dp")
    tokens, channels = vbuf.shape
    half = tokens // 2
    wrows = weight.shape[0]
    pairs = channels // LANES

    load_value = pltpu.make_async_copy(value, vbuf, load_sem.at[0])
    load_gain = pltpu.make_async_copy(gain, gainbuf, load_sem.at[1])
    load_nbias = pltpu.make_async_copy(nbias, nbiasbuf, load_sem.at[2])
    load_gate = pltpu.make_async_copy(gate, gbuf, load_sem.at[3])
    load_mbias = pltpu.make_async_copy(mbias, mbiasbuf, load_sem.at[4])
    own_rows = full.at[pl.ds(pl.multiple_of(row * wrows, wrows), wrows), :]
    load_weight = pltpu.make_async_copy(weight, own_rows, load_sem.at[5])
    load_value.start()
    load_gain.start()
    load_nbias.start()
    load_weight.start()
    load_mbias.start()
    load_gate.start()

    barrier = pltpu.get_barrier_semaphore()
    late = 2 * ((me * tokens + half) % SPAN) // SPAN
    peers = [partner(me, k + late * (n - 2 * k), n) for k in range(n - 1, 0, -1)]
    for peer in peers:
        pl.semaphore_signal(barrier, inc=1, device_id={"sp": peer})
    for j in range(1, dp):
        pl.semaphore_signal(barrier, inc=1, device_id={"dp": lax.rem(row + j, dp)})

    load_value.wait()
    load_gain.wait()
    load_nbias.wait()
    lower = lax.broadcasted_iota(jnp.int32, (ROWS, LANES), 1) < GROUP_DIM

    def normed_rows(start):
        x = jax.nn.gelu(vbuf[pl.ds(start, ROWS), :].astype(jnp.float32))
        shifted = x - jnp.mean(x, axis=-1, keepdims=True)
        variance = jnp.mean(shifted * shifted, axis=-1, keepdims=True)
        return shifted * lax.rsqrt(variance + epsilon) * gainbuf[...] + nbiasbuf[...]

    for r in range(0, half, ROWS):
        top = normed_rows(r)
        bottom = normed_rows(half + r)
        for j in range(pairs):
            t = top[:, j * LANES:(j + 1) * LANES]
            b = bottom[:, j * LANES:(j + 1) * LANES]
            s1[2 * j, pl.ds(r, ROWS), :] = jnp.where(lower, t, pltpu.roll(b, GROUP_DIM, 1)).astype(jnp.bfloat16)
            s1[2 * j + 1, pl.ds(r, ROWS), :] = jnp.where(lower, pltpu.roll(t, GROUP_DIM, 1), b).astype(jnp.bfloat16)

    pl.semaphore_wait(barrier, n - 1 + dp - 1)

    sends = []
    for k, peer in enumerate(peers):
        copy = pltpu.make_async_remote_copy(
            src_ref=s1.at[peer], dst_ref=r1.at[me], send_sem=send1.at[k], recv_sem=recv1.at[me], device_id={"sp": peer},
        )
        copy.start()
        sends.append(copy)
    pltpu.make_async_copy(s1.at[me], r1.at[me], recv1.at[me]).start()

    def give_back(s):
        return pltpu.make_async_remote_copy(
            src_ref=s2.at[s], dst_ref=r2.at[me], send_sem=send2.at[s], recv_sem=recv2.at[me], device_id={"sp": s},
        )

    wcopies = []
    for j in range(1, dp):
        copy = pltpu.make_async_remote_copy(
            src_ref=weight, dst_ref=own_rows, send_sem=wsend.at[j], recv_sem=wrecv.at[row],
            device_id={"dp": lax.rem(row + j, dp)},
        )
        copy.start()
        wcopies.append(copy)

    load_gate.wait()
    for r in range(0, tokens, ROWS):
        act[pl.ds(r, ROWS), :] = jax.nn.gelu(gbuf[pl.ds(r, ROWS), :].astype(jnp.float32))
    load_mbias.wait()
    for q in range(0, SPAN, LANES):
        bcol[pl.ds(q, LANES), :] = jnp.transpose(jnp.broadcast_to(mbiasbuf[:, q:q + LANES], (LANES, LANES)))
    xbuf[:, xbuf.shape[1] - LANES:] = jnp.zeros((SPAN, LANES), jnp.bfloat16)

    load_weight.wait()
    for j in range(1, dp):
        other = lax.rem(row + j, dp)
        rows_of = full.at[pl.ds(pl.multiple_of(other * wrows, wrows), wrows), :]
        pltpu.make_async_copy(weight, rows_of, wrecv.at[other]).wait()
    for q in range(0, SPAN, tile):
        block = full[pl.ds(q, tile), pl.ds(q, tile)].astype(jnp.float32)
        keep = lax.broadcasted_iota(jnp.int32, (tile, tile), 1) <= lax.broadcasted_iota(jnp.int32, (tile, tile), 0)
        full[pl.ds(q, tile), pl.ds(q, tile)] = jnp.where(keep, block, 0.0).astype(jnp.bfloat16)

    waited, returned = set(), set()
    for q in range(0, SPAN, tile):
        for s in range(n):
            runs = segments(s, tokens)
            if s in waited or min(p for _, _, _, _, p in runs) >= q + tile:
                continue
            waited.add(s)
            pltpu.make_async_copy(s1.at[s], r1.at[s], recv1.at[s]).wait()
            for a, r, length, block, p in runs:
                xbuf[p:p + length, block * GROUP_DIM:(block + 1) * GROUP_DIM] = (
                    r1[s, r:r + length, a * GROUP_DIM:(a + 1) * GROUP_DIM]
                )
        summed = jnp.dot(full[q:q + tile, :q + tile], xbuf[:q + tile, :], preferred_element_type=jnp.float32)
        column = bcol[q:q + tile, :]
        for j in range(0, xbuf.shape[1], LANES):
            ybuf[q:q + tile, j:j + LANES] = (summed[:, j:j + LANES] + column).astype(jnp.bfloat16)
        complete = []
        for s in range(n):
            runs = segments(s, tokens)
            if s in returned or max(p + length for _, _, length, _, p in runs) > q + tile:
                continue
            returned.add(s)
            complete.append(s)
            for a, r, length, block, p in runs:
                s2[s, r:r + length, a * GROUP_DIM:(a + 1) * GROUP_DIM] = (
                    ybuf[p:p + length, block * GROUP_DIM:(block + 1) * GROUP_DIM]
                )
        for s in complete:
            @pl.when(me != s)
            def _():
                give_back(s).start()

            @pl.when(me == s)
            def _():
                pltpu.make_async_copy(s2.at[s], r2.at[s], recv2.at[s]).start()

    for j in range(pairs):
        for s in (2 * j, 2 * j + 1):
            pltpu.make_async_copy(s2.at[s], r2.at[s], recv2.at[s]).wait()
        cols = slice(j * LANES, (j + 1) * LANES)
        for r in range(0, half, ROWS):
            e = r2[2 * j, r:r + ROWS, :].astype(jnp.float32)
            o = r2[2 * j + 1, r:r + ROWS, :].astype(jnp.float32)
            top = jnp.where(lower, e, pltpu.roll(o, GROUP_DIM, 1))
            bottom = jnp.where(lower, pltpu.roll(e, GROUP_DIM, 1), o)
            out[r:r + ROWS, cols] = (act[r:r + ROWS, cols] * top).astype(jnp.bfloat16)
            out[half + r:half + r + ROWS, cols] = (act[half + r:half + r + ROWS, cols] * bottom).astype(jnp.bfloat16)
    for copy in sends + wcopies:
        copy.wait_send()
    for s in range(n):
        @pl.when(me != s)
        def _():
            give_back(s).wait_send()


def solution(mesh):
    n, dp = mesh.shape["sp"], mesh.shape["dp"]

    def local(gate_input, value_input, norm_gain, norm_bias, mix_weight, mix_bias):
        _, tokens, channels = value_input.shape
        groups, wrows, span = mix_weight.shape
        assert groups == 1 and span == SPAN and channels == n * GROUP_DIM and tokens % (2 * ROWS) == 0
        half = tokens // 2
        blocks = n * tokens // SPAN
        width = -(-blocks * GROUP_DIM // LANES) * LANES
        packed = (n, half, 2 * GROUP_DIM)
        anywhere = pl.BlockSpec(memory_space=pl.ANY)
        bf16, f32 = jnp.bfloat16, jnp.float32
        dma = pltpu.SemaphoreType.DMA
        result = pl.pallas_call(
            functools.partial(kernel, n, dp, 256),
            out_shape=pltpu.VMEM((tokens, channels), bf16),
            in_specs=[anywhere] * 6,
            out_specs=pl.BlockSpec(memory_space=pltpu.VMEM),
            scratch_shapes=[
                pltpu.VMEM((tokens, channels), bf16),
                pltpu.VMEM((tokens, channels), bf16),
                pltpu.VMEM((1, channels), f32),
                pltpu.VMEM((1, channels), f32),
                pltpu.VMEM((1, SPAN), f32),
                pltpu.VMEM((tokens, channels), f32),
                pltpu.VMEM((SPAN, SPAN), bf16),
                pltpu.VMEM((SPAN, LANES), f32),
                pltpu.VMEM(packed, bf16),
                pltpu.VMEM(packed, bf16),
                pltpu.VMEM((SPAN, width), bf16),
                pltpu.VMEM((SPAN, width), bf16),
                pltpu.VMEM(packed, bf16),
                pltpu.VMEM(packed, bf16),
                dma((6,)),
                dma((dp,)),
                dma((dp,)),
                dma((n,)),
                dma((n,)),
                dma((n,)),
                dma((n,)),
            ],
            compiler_params=pltpu.CompilerParams(collective_id=0, has_side_effects=True),
        )(
            value_input[0], gate_input[0], norm_gain.reshape(1, channels), norm_bias.reshape(1, channels),
            mix_weight[0], mix_bias,
        )
        return result.reshape(1, tokens, channels)

    in_specs = (
        P("dp", "sp", None),
        P("dp", "sp", None),
        P(),
        P(),
        P("sp", "dp", None),
        P("sp", None),
    )
    return jax.shard_map(local, mesh=mesh, in_specs=in_specs, out_specs=P("dp", "sp", None), check_vma=False)
```

```python
import functools
import math

import jax
import jax.numpy as jnp
from jax import lax
from jax.experimental import pallas as pl
from jax.experimental.pallas import tpu as pltpu
from jax.sharding import PartitionSpec as P

GROUP_DIM = 64
SPAN = 1024
LANES = 128
ROWS = 16

epsilon = 1e-05


def partner(me, k, n):
    if n & (n - 1):
        return lax.rem(me + k, n)
    out = 0
    bit = 1
    while bit < n:
        out = out + ((me // bit + k // bit) % 2) * bit
        bit *= 2
    return out


def segments(source, rows):
    half = rows // 2
    runs = []
    for a in range(2):
        r = 0
        while r < half:
            position = source * rows + a * half + r
            block, p = divmod(position, SPAN)
            length = min(half - r, SPAN - p)
            runs.append((a, r, length, block, p))
            r += length
    return runs


def kernel(
    n, dp, tile, value, gate, gain, nbias, weight, mbias, out,
    vbuf, gbuf, gainbuf, nbiasbuf, mbiasbuf, act, full, bcol, s1, r1, xbuf, s2, r2,
    load_sem, wsend, wrecv, send1, recv1, send2, recv2,
):
    me = lax.axis_index("sp")
    row = lax.axis_index("dp")
    tokens, channels = vbuf.shape
    half = tokens // 2
    wrows = weight.shape[0]
    pairs = channels // LANES

    load_value = pltpu.make_async_copy(value, vbuf, load_sem.at[0])
    load_gain = pltpu.make_async_copy(gain, gainbuf, load_sem.at[1])
    load_nbias = pltpu.make_async_copy(nbias, nbiasbuf, load_sem.at[2])
    load_gate = pltpu.make_async_copy(gate, gbuf, load_sem.at[3])
    load_mbias = pltpu.make_async_copy(mbias, mbiasbuf, load_sem.at[4])
    own_rows = full.at[pl.ds(pl.multiple_of(row * wrows, wrows), wrows), :]
    load_weight = pltpu.make_async_copy(weight, own_rows, load_sem.at[5])
    load_value.start()
    load_gain.start()
    load_nbias.start()
    load_weight.start()
    load_mbias.start()
    load_gate.start()

    barrier = pltpu.get_barrier_semaphore()
    first = (me * tokens) % SPAN
    late = ((3 * first) // (2 * SPAN)) * (1 - (first + tokens - 1) // SPAN)
    peers = [partner(me, k + late * (n - 2 * k), n) for k in range(n - 1, 0, -1)]
    for peer in peers:
        pl.semaphore_signal(barrier, inc=1, device_id={"sp": peer})
    for j in range(1, dp):
        pl.semaphore_signal(barrier, inc=1, device_id={"dp": lax.rem(row + j, dp)})

    load_value.wait()
    load_gain.wait()
    load_nbias.wait()
    lower = lax.broadcasted_iota(jnp.int32, (ROWS, LANES), 1) < GROUP_DIM

    def normed_rows(start):
        x = jax.nn.gelu(vbuf[pl.ds(start, ROWS), :].astype(jnp.float32))
        shifted = x - jnp.mean(x, axis=-1, keepdims=True)
        variance = jnp.mean(shifted * shifted, axis=-1, keepdims=True)
        return shifted * lax.rsqrt(variance + epsilon) * gainbuf[...] + nbiasbuf[...]

    for r in range(0, half, ROWS):
        top = normed_rows(r)
        bottom = normed_rows(half + r)
        for j in range(pairs):
            t = top[:, j * LANES:(j + 1) * LANES]
            b = bottom[:, j * LANES:(j + 1) * LANES]
            s1[2 * j, pl.ds(r, ROWS), :] = jnp.where(lower, t, pltpu.roll(b, GROUP_DIM, 1)).astype(jnp.bfloat16)
            s1[2 * j + 1, pl.ds(r, ROWS), :] = jnp.where(lower, pltpu.roll(t, GROUP_DIM, 1), b).astype(jnp.bfloat16)

    pl.semaphore_wait(barrier, n - 1 + dp - 1)

    sends = []
    for k, peer in enumerate(peers):
        copy = pltpu.make_async_remote_copy(
            src_ref=s1.at[peer], dst_ref=r1.at[me], send_sem=send1.at[k], recv_sem=recv1.at[me], device_id={"sp": peer},
        )
        copy.start()
        sends.append(copy)
    pltpu.make_async_copy(s1.at[me], r1.at[me], recv1.at[me]).start()

    def give_back(s):
        return pltpu.make_async_remote_copy(
            src_ref=s2.at[s], dst_ref=r2.at[me], send_sem=send2.at[s], recv_sem=recv2.at[me], device_id={"sp": s},
        )

    wcopies = []
    for j in range(1, dp):
        copy = pltpu.make_async_remote_copy(
            src_ref=weight, dst_ref=own_rows, send_sem=wsend.at[j], recv_sem=wrecv.at[row],
            device_id={"dp": lax.rem(row + j, dp)},
        )
        copy.start()
        wcopies.append(copy)

    load_gate.wait()
    for r in range(0, tokens, ROWS):
        act[pl.ds(r, ROWS), :] = jax.nn.gelu(gbuf[pl.ds(r, ROWS), :].astype(jnp.float32))
    load_mbias.wait()
    for q in range(0, SPAN, LANES):
        bcol[pl.ds(q, LANES), :] = jnp.transpose(jnp.broadcast_to(mbiasbuf[:, q:q + LANES], (LANES, LANES)))
    xbuf[...] = jnp.zeros_like(xbuf)

    load_weight.wait()
    for j in range(1, dp):
        other = lax.rem(row + j, dp)
        rows_of = full.at[pl.ds(pl.multiple_of(other * wrows, wrows), wrows), :]
        pltpu.make_async_copy(weight, rows_of, wrecv.at[other]).wait()
    for q in range(0, SPAN, tile):
        block = full[pl.ds(q, tile), pl.ds(q, tile)].astype(jnp.float32)
        keep = lax.broadcasted_iota(jnp.int32, (tile, tile), 1) <= lax.broadcasted_iota(jnp.int32, (tile, tile), 0)
        full[pl.ds(q, tile), pl.ds(q, tile)] = jnp.where(keep, block, 0.0).astype(jnp.bfloat16)
        if q + tile < SPAN:
            full[q:q + tile, q + tile:] = jnp.zeros((tile, SPAN - q - tile), jnp.bfloat16)

    waited = set()
    last = {s: max(p + length for _, _, length, _, p in segments(s, tokens)) for s in range(n)}
    for s in sorted(range(n), key=last.get):
        for block in sorted({run[3] for run in segments(s, tokens)}):
            mine = [run for run in segments(s, tokens) if run[3] == block]
            begin = min(run[4] for run in mine)
            end = max(run[4] + run[2] for run in mine)
            for source in range(n):
                runs = segments(source, tokens)
                if source in waited or all(run[3] != block or run[4] >= end for run in runs):
                    continue
                waited.add(source)
                pltpu.make_async_copy(s1.at[source], r1.at[source], recv1.at[source]).wait()
                for a, r, length, into, p in runs:
                    xbuf[into, p:p + length, :] = r1[source, r:r + length, a * GROUP_DIM:(a + 1) * GROUP_DIM]
            depth = -(-end // LANES) * LANES
            summed = jnp.dot(full[begin:end, :depth], xbuf[block, :depth, :], preferred_element_type=jnp.float32)
            mixed = (summed + bcol[begin:end, :GROUP_DIM]).astype(jnp.bfloat16)
            for a, r, length, _, p in mine:
                s2[s, r:r + length, a * GROUP_DIM:(a + 1) * GROUP_DIM] = mixed[p - begin:p - begin + length, :]

        @pl.when(me != s)
        def _():
            give_back(s).start()

        @pl.when(me == s)
        def _():
            pltpu.make_async_copy(s2.at[s], r2.at[s], recv2.at[s]).start()

    for j in range(pairs):
        for s in (2 * j, 2 * j + 1):
            pltpu.make_async_copy(s2.at[s], r2.at[s], recv2.at[s]).wait()
        cols = slice(j * LANES, (j + 1) * LANES)
        for r in range(0, half, ROWS):
            e = r2[2 * j, r:r + ROWS, :].astype(jnp.float32)
            o = r2[2 * j + 1, r:r + ROWS, :].astype(jnp.float32)
            top = jnp.where(lower, e, pltpu.roll(o, GROUP_DIM, 1))
            bottom = jnp.where(lower, pltpu.roll(e, GROUP_DIM, 1), o)
            out[r:r + ROWS, cols] = (act[r:r + ROWS, cols] * top).astype(jnp.bfloat16)
            out[half + r:half + r + ROWS, cols] = (act[half + r:half + r + ROWS, cols] * bottom).astype(jnp.bfloat16)
    for copy in sends + wcopies:
        copy.wait_send()
    for s in range(n):
        @pl.when(me != s)
        def _():
            give_back(s).wait_send()


def solution(mesh):
    n, dp = mesh.shape["sp"], mesh.shape["dp"]

    def local(gate_input, value_input, norm_gain, norm_bias, mix_weight, mix_bias):
        _, tokens, channels = value_input.shape
        groups, wrows, span = mix_weight.shape
        assert groups == 1 and span == SPAN and channels == n * GROUP_DIM and tokens % (2 * ROWS) == 0
        half = tokens // 2
        blocks = n * tokens // SPAN
        packed = (n, half, 2 * GROUP_DIM)
        anywhere = pl.BlockSpec(memory_space=pl.ANY)
        bf16, f32 = jnp.bfloat16, jnp.float32
        dma = pltpu.SemaphoreType.DMA
        result = pl.pallas_call(
            functools.partial(kernel, n, dp, 256),
            out_shape=pltpu.VMEM((tokens, channels), bf16),
            in_specs=[anywhere] * 6,
            out_specs=pl.BlockSpec(memory_space=pltpu.VMEM),
            scratch_shapes=[
                pltpu.VMEM((tokens, channels), bf16),
                pltpu.VMEM((tokens, channels), bf16),
                pltpu.VMEM((1, channels), f32),
                pltpu.VMEM((1, channels), f32),
                pltpu.VMEM((1, SPAN), f32),
                pltpu.VMEM((tokens, channels), f32),
                pltpu.VMEM((SPAN, SPAN), bf16),
                pltpu.VMEM((SPAN, LANES), f32),
                pltpu.VMEM(packed, bf16),
                pltpu.VMEM(packed, bf16),
                pltpu.VMEM((blocks, SPAN, GROUP_DIM), bf16),
                pltpu.VMEM(packed, bf16),
                pltpu.VMEM(packed, bf16),
                dma((6,)),
                dma((dp,)),
                dma((dp,)),
                dma((n,)),
                dma((n,)),
                dma((n,)),
                dma((n,)),
            ],
            compiler_params=pltpu.CompilerParams(collective_id=0, has_side_effects=True),
        )(
            value_input[0], gate_input[0], norm_gain.reshape(1, channels), norm_bias.reshape(1, channels),
            mix_weight[0], mix_bias,
        )
        return result.reshape(1, tokens, channels)

    in_specs = (
        P("dp", "sp", None),
        P("dp", "sp", None),
        P(),
        P(),
        P("sp", "dp", None),
        P("sp", None),
    )
    return jax.shard_map(local, mesh=mesh, in_specs=in_specs, out_specs=P("dp", "sp", None), check_vma=False)
```
